512 devices in a mesh: grp: 2 (over y), sp: 32 (over z, core), tp: 8 (over x).
Axes of the slice: x: 8, y: 2, z: 16, core: 2. Of those that a mesh axis runs over, the one named last changes fastest.
The devices are a block of a 8x8x16 slice.
Arguments:
- tokens: bfloat16 [8, 4096, 4096], P('grp', 'sp'), parts along dimension 0, may hold values from -9 to 9
- w_forget: bfloat16 [4096, 4096], P('sp', 'tp'), may hold values from -0.09375 to 0.09375
- w_value: bfloat16 [4096, 4096], P('sp', 'tp'), may hold values from -0.09375 to 0.09375
- lower_bound: float32 [4096], P('tp'), may hold values from 0.25 to 1
- decay_shift: float32 [8, 4096, 32], P('grp', 'sp', 'tp'), parts along dimension 0, may hold values from -1 to 0
- queries: bfloat16 [8, 4096], P('grp', 'tp'), parts along dimension 0, may hold values from -6 to 6
- read_gain: float32 [4096], P('tp'), may hold values from 0.1 to 1.9
Outputs:
- cache_out: bfloat16 [8, 32, 16384], P('grp', 'tp', 'sp'), parts along dimension 0
- first_read: bfloat16 [8, 4096], P('grp', 'tp'), parts along dimension 0
The draws below stay inside these ranges and needn't reach their ends.
There are 2 independent parts, one for each index of `grp`. The reference program is written for one: setup_inputs(seed, part) draws one part's arguments, and reference() takes and returns one part's arrays. A program takes and returns all parts, laid end to end along the dimension named above; an argument that names none is the same for every part. Nothing has to cross between parts.
All inputs are finite; a program needn't handle non-finite values.
Results may differ from the reference program's by a relative error of at most 0.01.
Values may be sent and summed in bfloat16 or wider, within the bound.
A program may use at most 128 MiB of HBM per device.

```python
import jax
import jax.numpy as jnp
from jax import lax

D = 4096
ATTENTION_UNITS = 32
DK = 128
DV = 128
INPUT_SEQUENCES = 4
SPAN = 128
SEQUENCE_SPAN = 4096


def draw_tokens(key, part):
    first_key = jax.random.fold_in(key, 11)
    lookup_vector_two = jax.random.fold_in(key, 12)
    noise_rows = jax.random.normal(first_key, (INPUT_SEQUENCES, SEQUENCE_SPAN, D), jnp.float32)
    block_means = jax.random.normal(lookup_vector_two, (INPUT_SEQUENCES, SEQUENCE_SPAN // SPAN, D), jnp.float32)
    noise_rows = jnp.clip(noise_rows, -5.0, 5.0)
    block_means = jnp.clip(block_means, -4.0, 4.0)
    return (noise_rows + jnp.repeat(block_means, SPAN, axis=1)).astype(jnp.bfloat16)


def draw_lower_bound(key, part):
    first_key = jax.random.fold_in(key, 21)
    lookup_vector_two = jax.random.fold_in(key, 22)
    lookup_vector_three = jax.random.fold_in(key, 23)
    slow_share = 0.5
    slow_heads = jax.random.uniform(first_key, (ATTENTION_UNITS,), jnp.float32) < slow_share
    slow_value = 1.0 - jax.random.uniform(lookup_vector_two, (ATTENTION_UNITS,), jnp.float32, 0.2, 0.6) / SEQUENCE_SPAN
    fast_value = 1.0 - jax.random.uniform(lookup_vector_three, (ATTENTION_UNITS,), jnp.float32, 3.0, 6.0) / SPAN
    bound_heads = jnp.where(slow_heads, slow_value, fast_value)
    return jnp.repeat(bound_heads, DK).astype(jnp.float32)


def draw_decay_shift(key, part):
    first_key = jax.random.fold_in(key, 31)
    lookup_vector_two = jax.random.fold_in(key, 32)
    lookup_vector_three = jax.random.fold_in(key, 33)
    rate_block = jnp.exp(jax.random.uniform(first_key, (INPUT_SEQUENCES, SEQUENCE_SPAN // SPAN, ATTENTION_UNITS), jnp.float32, jnp.log(0.25), jnp.log(1.25)))
    constant_payload = -jnp.repeat(rate_block, SPAN, axis=1) / SEQUENCE_SPAN
    segment_number = jax.random.uniform(lookup_vector_two, (INPUT_SEQUENCES, SEQUENCE_SPAN, ATTENTION_UNITS), jnp.float32) < 2.0 / SEQUENCE_SPAN
    segment_size = jnp.log(jax.random.uniform(lookup_vector_three, (INPUT_SEQUENCES, SEQUENCE_SPAN, ATTENTION_UNITS), jnp.float32, 0.5, 0.8))
    return (constant_payload + jnp.where(segment_number, segment_size, 0.0)).astype(jnp.float32)


def levels(stream_key, dims, cuts, least, top_value):
    def one(dim, shards_of):
        draws = jax.random.uniform(jax.random.fold_in(jax.random.fold_in(stream_key, 6), dim), (shards_of,), jnp.float32, least / len(cuts), top_value / len(cuts))
        return jnp.repeat(jnp.exp(draws), dims[dim] // shards_of).reshape((-1,) + (1,) * (len(dims) - dim - 1))

    gain = one(*cuts[0])
    for cut in cuts[1:]:
        gain = gain * one(*cut)
    return gain


def bell_draw(rng, extent, deviation, reach, cuts=(), dtype=jnp.bfloat16):
    result = jax.random.normal(rng, extent, jnp.float32) * deviation
    if len(cuts) > 0:
        result = levels(rng, extent, cuts, -0.22, 0.18) * result
    return jnp.clip(result, min=-reach, max=reach).astype(dtype)


def setup_inputs(seed: int = 0, part: int = 0) -> dict:
    arg_keys = jax.random.split(jax.random.key(seed), 8)
    part_keys = jax.random.split(jax.random.fold_in(arg_keys[7], part), 8)
    tokens = draw_tokens(jax.random.fold_in(jax.random.fold_in(arg_keys[7], part), 71), part)
    w_forget = bell_draw(arg_keys[1], (D, ATTENTION_UNITS * DK), D ** -0.5, 0.09375, ((0, 32), (1, 8)))
    w_value = bell_draw(arg_keys[2], (D, ATTENTION_UNITS * DV), D ** -0.5, 0.09375, ((0, 32), (1, 8)))
    lower_bound = draw_lower_bound(jax.random.fold_in(arg_keys[7], 71), part)
    decay_shift = draw_decay_shift(jax.random.fold_in(jax.random.fold_in(arg_keys[7], part), 71), part)
    queries = bell_draw(part_keys[5], (INPUT_SEQUENCES, ATTENTION_UNITS * DK), 1.0, 6.0, ((1, 8),))
    read_gain = jnp.clip(1.0 + 0.18 * jax.random.normal(arg_keys[6], (ATTENTION_UNITS * DV,), jnp.float32), 0.1, 1.9)
    return {"tokens": tokens, "w_forget": w_forget, "w_value": w_value, "lower_bound": lower_bound, "decay_shift": decay_shift, "queries": queries, "read_gain": read_gain}


def one_sequence(tok_rows, shift_rows, w_forget, w_value, lower_bound):
    pre_gate = jnp.dot(tok_rows, w_forget, preferred_element_type=jnp.float32)
    values = jnp.dot(tok_rows, w_value, preferred_element_type=jnp.float32).astype(jnp.bfloat16)
    low_bound = lower_bound[None, :]
    log_forget = jnp.logaddexp(jnp.log(low_bound), jnp.log1p(-low_bound) + jax.nn.log_sigmoid(pre_gate))
    log_forget = log_forget.reshape(SEQUENCE_SPAN, ATTENTION_UNITS, DK) + shift_rows[:, :, None]
    key_gates = ((1.0 - low_bound) * jax.nn.sigmoid(-pre_gate)).reshape(SEQUENCE_SPAN, ATTENTION_UNITS, DK)
    span_count = SEQUENCE_SPAN // SPAN
    blocked = log_forget.reshape(span_count, SPAN, ATTENTION_UNITS, DK)
    inclusive = jnp.cumsum(blocked, axis=1)
    totals = inclusive[:, -1]
    weighted = (key_gates.reshape(span_count, SPAN, ATTENTION_UNITS, DK) * jnp.exp(totals[:, None] - inclusive)).astype(jnp.bfloat16)
    span_values = values.reshape(span_count, SPAN, ATTENTION_UNITS, DV)
    span_states = jnp.einsum('bthk,bthv->bhkv', weighted.astype(jnp.float32), span_values.astype(jnp.float32))
    suffix = jnp.cumsum(totals[::-1], axis=0)[::-1] - totals
    return lax.optimization_barrier(jnp.sum(jnp.exp(suffix)[..., None] * span_states, axis=0))

def reference(tokens, w_forget, w_value, lower_bound, decay_shift, queries, read_gain):

    def per_prompt(operands):
        return one_sequence(operands[0], operands[1], w_forget, w_value, lower_bound)
    final_state = lax.map(per_prompt, (tokens, decay_shift))
    cache_out = final_state.reshape(INPUT_SEQUENCES, ATTENTION_UNITS, DK * DV).astype(jnp.bfloat16)
    query_act = jax.nn.silu(queries.astype(jnp.float32)).reshape(INPUT_SEQUENCES, ATTENTION_UNITS, DK)
    total_read = jnp.einsum('shk,shkv->shv', query_act, final_state, precision=lax.Precision.HIGHEST)
    scaled = total_read * lax.rsqrt(lax.optimization_barrier(jnp.mean(total_read * total_read, axis=-1, keepdims=True)) + 1e-06)
    first_read = (scaled * read_gain.reshape(ATTENTION_UNITS, DV)).reshape(INPUT_SEQUENCES, ATTENTION_UNITS * DV).astype(jnp.bfloat16)
    return (cache_out, first_read)
```

```python
import functools

import jax
import jax.numpy as jnp
from jax import lax
from jax.experimental import pallas as pl
from jax.experimental.pallas import tpu as pltpu
from jax.sharding import PartitionSpec as P

DK = 128
DV = 128
F32 = jnp.float32
BF16 = jnp.bfloat16

LONE_ROWS = (32, 48)
PIECE_ROWS = (32, 16)
NT = (((1,), (1,)), ((), ()))


def split3(x):
    hi = x.astype(BF16)
    rest = x - hi.astype(F32)
    mid = rest.astype(BF16)
    lo = (rest - mid.astype(F32)).astype(BF16)
    return hi, mid, lo


def exact_dot(ones, x, dims):
    total = None
    for part in split3(x):
        term = lax.dot_general(ones, part, dims, preferred_element_type=F32)
        total = term if total is None else total + term
    return total


def kernel(
    nz,
    lone,
    piece,
    tok_hbm,
    wf_hbm,
    wv_hbm,
    lb_ref,
    shift_ref,
    q_ref,
    gain_ref,
    cache_ref,
    read_ref,
    tok,
    w,
    acc,
    amat,
    upper,
    shift_suf,
    tot,
    sib_tot,
    chip_tot,
    far_tot,
    suf_half,
    suf,
    rows16,
    dcol,
    qcol,
    dec_state,
    pay,
    sib_pay,
    comb,
    comb_b,
    far_state,
    rloc,
    rsib,
    rchip,
    far_read,
    rtot,
    local_sem,
    rs0,
    ss0,
    rs1,
    ss1,
    yr,
    ys,
    dr,
    ds,
    sib_r,
    sib_s,
    ft_r,
    ft_s,
    fs_r,
    fs_s,
    fr_r,
    fr_s,
):
    seqs, heads = cache_ref.shape[0], cache_ref.shape[1]
    span = DK
    shard = wf_hbm.shape[0]
    width = wf_hbm.shape[1]
    own = DK // (2 * nz)
    group = own * heads
    half = nz // 2
    sp = lax.axis_index("sp")
    z = sp // 2
    c = sp % 2
    grp = lax.axis_index("grp")
    gpar = grp % 2
    partner = {"grp": grp + 1 - 2 * gpar}
    sibling = {"sp": sp + 1 - 2 * c}

    def chip(zz):
        return {"sp": 2 * zz + c}

    def wrap(v):
        return lax.rem(v + 2 * nz, nz)

    pieces = [(shard - lone[p]) // piece[p] for p in (0, 1)]
    firsts = [(n + 1) // 2 for n in pieces]
    zrecv = (rs0, rs1)
    zsend = (ss0, ss1)

    def ring(p, way, k, j, sending):
        sign = -1 if way == 0 else 1
        at = k if sending else k + 1
        slot = wrap(z + sign * at)
        row = pl.multiple_of(c * shard + gpar * lone[p] + j * piece[p], 16)
        ref = w.at[p, slot, pl.ds(row, piece[p]), :]
        return pltpu.make_async_remote_copy(
            src_ref=ref,
            dst_ref=ref,
            send_sem=zsend[p].at[way, k, j],
            recv_sem=zrecv[p].at[way, k, j],
            device_id=chip(wrap(z - sign)),
            device_id_type=pl.DeviceIdType.MESH,
        )

    def in_last(p, way, j):
        return j < firsts[p] if way == 0 else j >= firsts[p]

    def lone_copy(p, rel, sending):
        side = gpar if sending else 1 - gpar
        row = pl.multiple_of(c * shard + side * (shard - lone[p]), 16)
        ref = w.at[p, wrap(z - rel), pl.ds(row, lone[p]), :]
        return pltpu.make_async_remote_copy(
            src_ref=ref,
            dst_ref=ref,
            send_sem=ys.at[p, rel],
            recv_sem=yr.at[p, rel],
            device_id=partner,
            device_id_type=pl.DeviceIdType.MESH,
        )

    def pair_copy(p, rel, sending):
        side = c if sending else 1 - c
        row = pl.multiple_of(side * shard, 16)
        ref = w.at[p, wrap(z - rel), pl.ds(row, shard), :]
        return pltpu.make_async_remote_copy(
            src_ref=ref,
            dst_ref=ref,
            send_sem=ds.at[p, rel],
            recv_sem=dr.at[p, rel],
            device_id=sibling,
            device_id_type=pl.DeviceIdType.MESH,
        )

    def sib_copy(i, src, dst):
        return pltpu.make_async_remote_copy(
            src_ref=src,
            dst_ref=dst,
            send_sem=sib_s.at[i],
            recv_sem=sib_r.at[i],
            device_id=sibling,
            device_id_type=pl.DeviceIdType.MESH,
        )

    def far_copy(src, dst, send, recv, dz, sign):
        return pltpu.make_async_remote_copy(
            src_ref=src,
            dst_ref=dst,
            send_sem=send.at[dz],
            recv_sem=recv.at[dz],
            device_id=chip(wrap(z + sign * dz)),
            device_id_type=pl.DeviceIdType.MESH,
        )

    own_rows = pl.ds(pl.multiple_of(c * shard, 16), shard)
    copies = (
        pltpu.make_async_copy(wf_hbm, w.at[0, z, own_rows, :], local_sem.at[0]),
        pltpu.make_async_copy(wv_hbm, w.at[1, z, own_rows, :], local_sem.at[1]),
        pltpu.make_async_copy(tok_hbm, tok, local_sem.at[2]),
    )
    for cp in copies:
        cp.start()
    barrier = pltpu.get_barrier_semaphore()
    for peer in (chip(wrap(z + 1)), chip(wrap(z - 1)), sibling, partner):
        pl.semaphore_signal(
            barrier, inc=1, device_id=peer, device_id_type=pl.DeviceIdType.MESH
        )
    copies[0].wait()
    pl.semaphore_wait(barrier, 4)

    def own_sends(p):
        for j in range(pieces[p]):
            for way in (0, 1):
                ring(p, way, 0, j, True).start()
        pair_copy(p, 0, True).start()

    own_sends(0)
    copies[1].wait()

    acc[...] = jnp.zeros(acc.shape, F32)
    r_i = lax.broadcasted_iota(jnp.int32, (span, span), 0)
    c_i = lax.broadcasted_iota(jnp.int32, (span, span), 1)
    upper[...] = jnp.where(c_i > r_i, 1.0, 0.0).astype(BF16)
    shift_suf[...] = exact_dot(upper[...], shift_ref[...], NT)

    nrow = 2 * nz * group

    def perm():
        r = lax.broadcasted_iota(jnp.int32, (nrow, DK), 0)
        k = lax.broadcasted_iota(jnp.int32, (nrow, DK), 1)
        side = r // (nz * group)
        inner = r % (nz * group)
        key = (inner // group) * (2 * own) + side * own + (inner % group) // heads
        return jnp.where(k == key, 1.0, 0.0).astype(BF16)

    def head_of_row(cols):
        r = lax.broadcasted_iota(jnp.int32, (nrow, cols), 0)
        return r % heads

    def columns(x16, out):
        spread = exact_dot(perm(), x16, NT)
        head = head_of_row(spread.shape[1])
        lane = lax.broadcasted_iota(jnp.int32, spread.shape, 1)
        for s in range(seqs):
            col = jnp.sum(
                jnp.where(lane == s * heads + head, spread, 0.0), axis=1, keepdims=True
            )
            out[s] = jnp.broadcast_to(col, (nrow, DV))

    query = q_ref[...].astype(F32)
    query = query * jax.nn.sigmoid(query)
    for s in range(seqs):
        for h in range(heads):
            rows16[s * heads + h : s * heads + h + 1, :] = query[
                s : s + 1, h * DK : (h + 1) * DK
            ]
    columns(rows16[...], qcol)
    copies[2].wait()

    def gate(s):
        rows = pl.ds(pl.multiple_of(s * span, span), span)
        pre = acc[0, rows, :]
        key_gate = (1.0 - lb_ref[...]) * jax.nn.sigmoid(-pre)
        log_forget = jnp.log1p(-key_gate)
        later = exact_dot(upper[...], log_forget, (((1,), (0,)), ((), ())))
        total = jnp.sum(log_forget, axis=0, keepdims=True)
        lane = lax.broadcasted_iota(jnp.int32, shift_suf.shape, 1)
        head = head_of_row(span)
        for h in range(heads):
            cols = slice(h * DK, (h + 1) * DK)
            idx = s * heads + h
            shift = jnp.sum(
                jnp.where(lane == idx, shift_suf[...], 0.0), axis=1, keepdims=True
            )
            weighted = (key_gate[:, cols] * jnp.exp(later[:, cols] + shift)).astype(BF16)
            turned = lax.dot_general(perm(), weighted, NT, preferred_element_type=F32)
            amat[s, :, cols] = jnp.where(head == h, turned, 0.0).astype(BF16)
            tot[pl.ds(idx, 1), :] = total[:, cols] + jnp.sum(
                shift_ref[pl.ds(idx, 1), :], axis=1, keepdims=True
            )

    rows_half = seqs * heads // 2
    mine = pl.ds(pl.multiple_of(c * rows_half, 8), rows_half)
    theirs = pl.ds(pl.multiple_of((1 - c) * rows_half, 8), rows_half)
    tot_copy = sib_copy(0, tot, sib_tot)

    def send_totals():
        chip_tot[...] = tot[...] + sib_tot[...]

        @pl.loop(1, nz)
        def _(dz):
            @pl.when(z >= dz)
            def _():
                far_copy(chip_tot.at[mine, :], far_tot.at[z], ft_s, ft_r, dz, -1).start()

    suf_copy = sib_copy(1, suf_half.at[mine, :], suf_half.at[mine, :])
    suf_wait = sib_copy(1, suf_half.at[theirs, :], suf_half.at[theirs, :])

    def take_totals():
        suf_half[mine, :] = jnp.zeros((rows_half, DK), F32)

        @pl.loop(1, nz)
        def _(dz):
            @pl.when(z + dz < nz)
            def _():
                far_copy(
                    chip_tot.at[mine, :], far_tot.at[wrap(z + dz)], ft_s, ft_r, dz, -1
                ).wait_recv()
                suf_half[mine, :] += far_tot[wrap(z + dz)]

        suf_copy.start()

    def finish_suffix():
        suf_wait.wait_recv()
        suf[...] = jnp.exp(
            suf_half[...] + jnp.where(c == 0, 1.0, 0.0) * sib_tot[...]
        )
        columns(suf[...], dcol)

    def stage1(p, s):
        for j in range(pieces[p]):
            for way in (0, 1):

                @pl.when(jnp.logical_or(s < half, in_last(p, way, j)))
                def _():
                    ring(p, way, s - 1, j, False).wait_recv()

                @pl.when(
                    jnp.logical_or(
                        s < half - 1, jnp.logical_and(s == half - 1, in_last(p, way, j))
                    )
                )
                def _():
                    ring(p, way, s, j, True).start()

        if lone[p]:
            lone_copy(p, s, True).start()

            @pl.when(s < half)
            def _():
                lone_copy(p, nz - s, True).start()

    def stage2(p, s):
        if lone[p]:
            lone_copy(p, s, False).wait_recv()
        pair_copy(p, s, True).start()

        @pl.when(s < half)
        def _():
            if lone[p]:
                lone_copy(p, nz - s, False).wait_recv()
            pair_copy(p, nz - s, True).start()

    def multiply(p, rel):
        pair_copy(p, rel, False).wait_recv()
        slot = wrap(z - rel)
        cols = pl.ds(pl.multiple_of(slot * 2 * shard, 2 * shard), 2 * shard)
        acc[p] += jnp.dot(tok[:, cols], w[p, slot], preferred_element_type=F32)

    gate_at = half + 2
    pairs = seqs // 2
    last = 2 * half + 3

    @pl.loop(0, last)
    def _(t):
        @pl.when(t == half)
        def _():
            own_sends(1)

        for p in (0, 1):
            s = t - p * half

            @pl.when(jnp.logical_and(s >= 1, s <= half))
            def _():
                stage1(p, s)

            @pl.when(jnp.logical_and(s >= 2, s <= half + 1))
            def _():
                stage2(p, s - 1)

        @pl.loop(0, 4)
        def _(item):
            p = item // 2
            way = item % 2
            s = t - p * half - 2
            ok = jnp.logical_and(s >= 0, s <= half)
            ok = jnp.logical_and(
                ok, jnp.logical_or(way == 0, jnp.logical_and(s >= 1, s < half))
            )

            @pl.when(ok)
            def _():
                multiply(p, jnp.where(way == 0, s, nz - s))

        @pl.when(jnp.logical_and(t >= gate_at, t < gate_at + 2))
        def _():
            @pl.loop(0, pairs)
            def _(i):
                gate((t - gate_at) * pairs + i)

        @pl.when(t == gate_at + 1)
        def _():
            tot_copy.start()

        @pl.when(t == gate_at + 2)
        def _():
            tot_copy.wait_recv()
            send_totals()

        @pl.when(t == last - 2)
        def _():
            take_totals()

        @pl.when(t == last - 1)
        def _():
            finish_suffix()

    for s in range(seqs):
        rows = slice(s * span, (s + 1) * span)
        values = jnp.concatenate(
            [
                acc[1, rows, h * DV : (h + 1) * DV].astype(BF16)
                for h in range(heads)
            ],
            axis=0,
        )
        state = jnp.dot(amat[s], values, preferred_element_type=F32) * dcol[s]
        part = state.reshape(2, nz, group, DV)
        dec_state[:, :, s * group : (s + 1) * group, :] = part
        pay[:, :, s * group : (s + 1) * group, :] = part.astype(BF16)
        read = jnp.sum((state * qcol[s]).reshape(nrow // 8, 8, DV), axis=0)
        for h in range(heads):
            row = read[h : h + 1]
            for again in range(h + heads, 8, heads):
                row = row + read[again : again + 1]
            rloc[s * heads + h : s * heads + h + 1, :] = row

    state_copy = sib_copy(2, pay.at[1 - c], sib_pay)
    read_copy = sib_copy(3, rloc, rsib)
    state_copy.start()
    read_copy.start()
    read_copy.wait_recv()
    rchip[...] = rloc[...] + rsib[...]
    state_copy.wait_recv()
    comb[...] = dec_state[c] + sib_pay[...].astype(F32)
    comb_b[...] = comb[...].astype(BF16)

    @pl.loop(1, nz)
    def _(dz):
        far_copy(comb_b.at[wrap(z + dz)], far_state.at[z], fs_s, fs_r, dz, 1).start()
        far_copy(rchip.at[mine, :], far_read.at[z], fr_s, fr_r, dz, 1).start()

    rtot[mine, :] = rchip[mine, :]
    comb[0] = comb[z]

    @pl.loop(1, nz)
    def _(dz):
        src = wrap(z - dz)
        far_copy(rchip.at[mine, :], far_read.at[src], fr_s, fr_r, dz, 1).wait_recv()
        rtot[mine, :] += far_read[src]

    final_copy = sib_copy(4, rtot.at[mine, :], rtot.at[mine, :])
    final_wait = sib_copy(4, rtot.at[theirs, :], rtot.at[theirs, :])
    final_copy.start()

    @pl.loop(1, nz)
    def _(dz):
        src = wrap(z - dz)
        far_copy(comb_b.at[0], far_state.at[src], fs_s, fs_r, dz, 1).wait_recv()
        comb[0] += far_state[src].astype(F32)

    final = comb[0]
    for s in range(seqs):
        for i in range(own):
            at = s * group + i * heads
            cache_ref[s, :, i * DV : (i + 1) * DV] = final[at : at + heads].astype(BF16)

    final_wait.wait_recv()
    total = rtot[...]
    scaled = total * lax.rsqrt(jnp.mean(total * total, axis=-1, keepdims=True) + 1e-06)
    for s in range(seqs):
        for h in range(heads):
            cols = slice(h * DV, (h + 1) * DV)
            at = s * heads + h
            read_ref[s : s + 1, cols] = (scaled[at : at + 1] * gain_ref[:, cols]).astype(BF16)

    for p in (0, 1):

        @pl.loop(0, half)
        def _(k):
            for way in (0, 1):
                for j in range(pieces[p]):

                    @pl.when(jnp.logical_or(k < half - 1, in_last(p, way, j)))
                    def _():
                        ring(p, way, k, j, True).wait_send()

        @pl.loop(0, nz)
        def _(rel):
            pair_copy(p, rel, True).wait_send()
            if lone[p]:

                @pl.when(rel >= 1)
                def _():
                    lone_copy(p, rel, True).wait_send()

    for cp in (tot_copy, suf_copy, state_copy, read_copy, final_copy):
        cp.wait_send()

    @pl.loop(1, nz)
    def _(dz):
        @pl.when(z >= dz)
        def _():
            far_copy(chip_tot.at[mine, :], far_tot.at[z], ft_s, ft_r, dz, -1).wait_send()

        far_copy(comb_b.at[wrap(z + dz)], far_state.at[z], fs_s, fs_r, dz, 1).wait_send()
        far_copy(rchip.at[mine, :], far_read.at[z], fr_s, fr_r, dz, 1).wait_send()


def shards(tokens, w_forget, w_value, lower_bound, decay_shift, queries, read_gain):
    seqs, span, feat = tokens.shape
    shard, width = w_forget.shape
    heads = width // DK
    nz = lax.axis_size("sp") // 2
    half = nz // 2
    own = DK // (2 * nz)
    group = own * heads
    nrow = 2 * nz * group
    n = seqs * heads
    lone = LONE_ROWS if lax.axis_size("grp") % 2 == 0 else (0, 0)
    pieces = [(shard - lone[p]) // PIECE_ROWS[p] for p in (0, 1)]
    dma = pltpu.SemaphoreType.DMA
    vmem = pl.BlockSpec(memory_space=pltpu.VMEM)
    anywhere = pl.BlockSpec(memory_space=pl.ANY)
    cache_out, first_read = pl.pallas_call(
        functools.partial(kernel, nz, lone, PIECE_ROWS),
        out_shape=(
            jax.ShapeDtypeStruct((seqs, heads, own * DV), BF16),
            jax.ShapeDtypeStruct((seqs, heads * DV), BF16),
        ),
        in_specs=[anywhere] * 3 + [vmem] * 4,
        out_specs=(vmem, vmem),
        scratch_shapes=[
            pltpu.VMEM((seqs * span, feat), BF16),
            pltpu.VMEM((2, nz, 2 * shard, width), BF16),
            pltpu.VMEM((2, seqs * span, width), F32),
            pltpu.VMEM((seqs, nrow, heads * span), BF16),
            pltpu.VMEM((span, span), BF16),
            pltpu.VMEM((span, n), F32),
            pltpu.VMEM((n, DK), F32),
            pltpu.VMEM((n, DK), F32),
            pltpu.VMEM((n, DK), F32),
            pltpu.VMEM((nz, n // 2, DK), F32),
            pltpu.VMEM((n, DK), F32),
            pltpu.VMEM((n, DK), F32),
            pltpu.VMEM((n, DK), F32),
            pltpu.VMEM((seqs, nrow, DV), F32),
            pltpu.VMEM((seqs, nrow, DV), F32),
            pltpu.VMEM((2, nz, seqs * group, DV), F32),
            pltpu.VMEM((2, nz, seqs * group, DV), BF16),
            pltpu.VMEM((nz, seqs * group, DV), BF16),
            pltpu.VMEM((nz, seqs * group, DV), F32),
            pltpu.VMEM((nz, seqs * group, DV), BF16),
            pltpu.VMEM((nz, seqs * group, DV), BF16),
            pltpu.VMEM((n, DV), F32),
            pltpu.VMEM((n, DV), F32),
            pltpu.VMEM((n, DV), F32),
            pltpu.VMEM((nz, n // 2, DV), F32),
            pltpu.VMEM((n, DV), F32),
            dma((3,)),
            dma((2, half, pieces[0])),
            dma((2, half, pieces[0])),
            dma((2, half, pieces[1])),
            dma((2, half, pieces[1])),
            dma((2, nz)),
            dma((2, nz)),
            dma((2, nz)),
            dma((2, nz)),
            dma((5,)),
            dma((5,)),
            dma((nz,)),
            dma((nz,)),
            dma((nz,)),
            dma((nz,)),
            dma((nz,)),
            dma((nz,)),
        ],
        compiler_params=pltpu.CompilerParams(
            collective_id=0, has_side_effects=True, vmem_limit_bytes=48 * 1024 * 1024
        ),
    )(
        tokens.reshape(seqs * span, feat),
        w_forget,
        w_value,
        lower_bound.reshape(1, width),
        decay_shift.transpose(0, 2, 1).reshape(n, span),
        queries,
        read_gain.reshape(1, heads * DV),
    )
    return cache_out, first_read


def solution(mesh):
    placed = (
        P("grp", "sp", None),
        P("sp", "tp"),
        P("sp", "tp"),
        P("tp"),
        P("grp", "sp", "tp"),
        P("grp", "tp"),
        P("tp"),
    )
    return jax.shard_map(
        shards,
        mesh=mesh,
        in_specs=placed,
        out_specs=(P("grp", "tp", "sp"), P("grp", "tp")),
        check_vma=False,
    )
```
